32 devices in a mesh: sp: 8 (over z, x), tp: 4 (over y, core).
Axes of the slice: x: 2, y: 2, z: 4, core: 2. Of those that a mesh axis runs over, the one named last changes fastest.
Arguments:
- residual: bfloat16 [1024, 2048], P('sp'), may hold values from -6 to 6
- query_narrow: bfloat16 [1024, 1024], P('sp', 'tp'), may hold values from -6 to 6
- keys_narrow: bfloat16 [1024, 1024], P('sp', 'tp'), may hold values from -6 to 6
- values_narrow: bfloat16 [1024, 1024], P('sp', 'tp'), may hold values from -6 to 6
- outgate_narrow: bfloat16 [1024, 1024], P('sp', 'tp'), may hold values from -6 to 6
- gates_narrow: float32 [4, 8, 1024], P(None, 'tp', 'sp'), may hold values from -4 to 100
- query_broad: bfloat16 [1024, 1024], P('sp', 'tp'), may hold values from -6 to 6
- keys_broad: bfloat16 [1024, 1024], P('sp', 'tp'), may hold values from -6 to 6
- values_broad: bfloat16 [1024, 1024], P('sp', 'tp'), may hold values from -6 to 6
- outgate_broad: bfloat16 [1024, 1024], P('sp', 'tp'), may hold values from -6 to 6
- gates_broad: float32 [4, 4, 1024], P(None, 'tp', 'sp'), may hold values from -4 to 100
- outproj_narrow: bfloat16 [1024, 2048], P('tp'), may hold values from -0.125 to 0.125
- outproj_broad: bfloat16 [1024, 2048], P('tp'), may hold values from -0.125 to 0.125
- norm_gain: bfloat16 [2048], replicated, may hold values from 0.099609375 to 1.8984375
- gate_weight: bfloat16 [2048, 5632], P('sp', 'tp'), may hold values from -0.125 to 0.125
- up_weight: bfloat16 [2048, 5632], P('sp', 'tp'), may hold values from -0.125 to 0.125
- down_weight: bfloat16 [2048, 5632], P('sp', 'tp'), may hold values from -0.078125 to 0.078125
Outputs:
- layer_out: bfloat16 [1024, 2048], P(('sp', 'tp'))
The draws below stay inside these ranges and needn't reach their ends.
All inputs are finite; a program needn't handle non-finite values.
Results may differ from the reference program's by a relative error of at most 0.0085.
Values may be sent and summed in bfloat16 or wider, within the bound.
No kernel may reach another device: no remote copies, remote signals or barrier semaphores. Data moves between devices by JAX's collectives and lax.ppermute only.
A program may use at most 192 MiB of HBM per device.

```python
import jax
import jax.numpy as jnp
from jax import lax

D = 2048
H_A = 8
DH_A = 128
H_B = 4
DH_B = 256
FF = 5632
TOK_DEV = 128
TOKENS = 1024
D_A = 1024
D_B = 1024
N_TP = 4


def gate_draw(key, number_of_heads):
    running_total = TOKENS
    every_key_row = jax.random.split(key, 9)
    in_gate = jnp.clip(jax.random.normal(every_key_row[0], (2, number_of_heads, running_total), jnp.float32), -4.0, 4.0)
    fast_share = 0.5
    fast = jax.random.uniform(every_key_row[4], (2, number_of_heads, 1)) < fast_share
    base_rate = jnp.where(fast, 1.0 / 40.0, 0.25 / running_total)
    block_count = running_total // TOK_DEV
    block_factor = jnp.exp(jax.random.uniform(every_key_row[5], (2, 1, block_count), jnp.float32, -0.7, 0.7))
    block_factor = jnp.repeat(block_factor, TOK_DEV, axis=2)
    rate = base_rate * block_factor * jnp.exp(0.5 * jax.random.normal(every_key_row[6], (2, number_of_heads, running_total), jnp.float32))
    forget_gate = -jnp.log(rate)
    spike_positions = jax.random.randint(every_key_row[7], (3,), 0, running_total)
    spike_flag = jnp.any(jnp.arange(running_total)[:, None] == spike_positions[None, :], axis=1)
    spike_magnitude = jax.random.uniform(every_key_row[8], (2, number_of_heads, running_total), jnp.float32, 0.0, 1.4)
    forget_gate = jnp.where(spike_flag[None, None, :], spike_magnitude, forget_gate)
    forget_gate = jnp.maximum(forget_gate, 0.0)
    return jnp.concatenate([in_gate, forget_gate], axis=0).astype(jnp.float32)


def draw_gates_narrow(key, part):
    return gate_draw(jax.random.fold_in(key, 11), H_A)


def draw_gates_broad(key, part):
    return gate_draw(jax.random.fold_in(key, 12), H_B)


def level_of(own_key, shape, shards, smallest, top_value):
    def one(axis_at, parts):
        heights = jax.random.uniform(jax.random.fold_in(jax.random.fold_in(own_key, 6), axis_at), (parts,), jnp.float32, smallest / len(shards), top_value / len(shards))
        return jnp.repeat(jnp.exp(heights), shape[axis_at] // parts).reshape((-1,) + (1,) * (len(shape) - axis_at - 1))

    level = one(*shards[0])
    for cut in shards[1:]:
        level = level * one(*cut)
    return level


def centred(key, shape, scale, most, cuts=(), kind=jnp.bfloat16):
    drawn = scale * jax.random.normal(key, shape, jnp.float32)
    if cuts:
        drawn = drawn * level_of(key, shape, cuts, -0.22, 0.18)
    return jnp.clip(drawn, -most, most).astype(kind)


def setup_inputs(seed: int = 0) -> dict:
    key_of = jax.random.split(jax.random.key(seed), 18)
    return {
        "residual": centred(key_of[0], (TOKENS, D), 1.0, 6.0, ((0, 8),)),
        "query_narrow": centred(key_of[1], (TOKENS, D_A), 1.0, 6.0, ((0, 8), (1, 4))),
        "keys_narrow": centred(key_of[2], (TOKENS, D_A), 1.0, 6.0, ((0, 8), (1, 4))),
        "values_narrow": centred(key_of[3], (TOKENS, D_A), 1.0, 6.0, ((0, 8), (1, 4))),
        "outgate_narrow": centred(key_of[4], (TOKENS, D_A), 1.0, 6.0, ((0, 8), (1, 4))),
        "gates_narrow": draw_gates_narrow(jax.random.fold_in(key_of[17], 71), 0),
        "query_broad": centred(key_of[6], (TOKENS, D_B), 1.0, 6.0, ((0, 8), (1, 4))),
        "keys_broad": centred(key_of[7], (TOKENS, D_B), 1.0, 6.0, ((0, 8), (1, 4))),
        "values_broad": centred(key_of[8], (TOKENS, D_B), 1.0, 6.0, ((0, 8), (1, 4))),
        "outgate_broad": centred(key_of[9], (TOKENS, D_B), 1.0, 6.0, ((0, 8), (1, 4))),
        "gates_broad": draw_gates_broad(jax.random.fold_in(key_of[17], 71), 0),
        "outproj_narrow": centred(key_of[11], (D_A, D), (D_A + D_B) ** -0.5, 0.125, ((0, 4),)),
        "outproj_broad": centred(key_of[12], (D_B, D), (D_A + D_B) ** -0.5, 0.125, ((0, 4),)),
        "norm_gain": jnp.clip(1.0 + 0.18 * jax.random.normal(key_of[13], (D,), jnp.float32), 0.099609375, 1.8984375).astype(jnp.bfloat16),
        "gate_weight": centred(key_of[14], (D, FF), D ** -0.5, 0.125, ((0, 8), (1, 4))),
        "up_weight": centred(key_of[15], (D, FF), D ** -0.5, 0.125, ((0, 8), (1, 4))),
        "down_weight": centred(key_of[16], (D, FF), FF ** -0.5, 0.078125, ((0, 8), (1, 4))),
    }


EPSILON = 1e-06
START_MAX = -1e+30

def rounded(values_in):
    return lax.optimization_barrier(values_in.astype(jnp.bfloat16)).astype(jnp.float32)

def empty_state(number_of_heads, head_width):
    return (jnp.zeros((number_of_heads, head_width, head_width), jnp.float32), jnp.zeros((number_of_heads, head_width), jnp.float32), jnp.full((number_of_heads,), START_MAX, jnp.float32), jnp.zeros((number_of_heads,), jnp.float32))

def combine(earlier_state, later_state):
    memory_early, normer_early, max_early, total_early = earlier_state
    memory_late, normer_late, max_late, total_late = later_state
    new_max = jnp.maximum(max_early + total_late, max_late)
    keep_early = jnp.exp(max_early + total_late - new_max)
    keep_late = jnp.exp(max_late - new_max)
    return (keep_early[:, None, None] * memory_early + keep_late[:, None, None] * memory_late, keep_early[:, None] * normer_early + keep_late[:, None] * normer_late, new_max, total_early + total_late)

def local_pass(query_rows, key_rows, value_rows, in_gate, log_forget):
    length = query_rows.shape[0]
    scaling = query_rows.shape[2] ** (-0.5)
    cumulative = jnp.cumsum(log_forget, axis=1)
    positions = jnp.arange(length)
    lower_tri = positions[:, None] >= positions[None, :]
    log_weight = jnp.where(lower_tri[None], cumulative[:, :, None] - cumulative[:, None, :] + in_gate[:, None, :], -jnp.inf)
    local_max = lax.optimization_barrier(jnp.max(log_weight, axis=2))
    query_float = query_rows.astype(jnp.float32)
    key_float = key_rows.astype(jnp.float32)
    value_float = value_rows.astype(jnp.float32)
    scores = jnp.einsum('thd,shd->hts', query_float, key_float) * scaling
    weighted = jnp.exp(log_weight - local_max[:, :, None]) * scores
    local_den = lax.optimization_barrier(jnp.sum(weighted, axis=2))
    local_num = jnp.einsum('hts,shd->thd', rounded(weighted), value_float)
    decay_total = cumulative[:, -1]
    toward_end = decay_total[:, None] - cumulative + in_gate
    end_max = lax.optimization_barrier(jnp.max(toward_end, axis=1))
    end_share = jnp.exp(toward_end - end_max[:, None])
    weighted_keys = jnp.transpose(end_share)[:, :, None] * key_float
    memory = jnp.einsum('shv,shk->hvk', value_float, rounded(weighted_keys))
    normer = lax.optimization_barrier(jnp.sum(weighted_keys, axis=0))
    return ((local_num, local_den, local_max, cumulative), (memory, normer, end_max, decay_total))

def finish(local, query_rows, carried):
    local_num, local_den, local_max, cumulative = local
    memory, normer, start_max, decay_total = carried
    scaling = query_rows.shape[2] ** (-0.5)
    query_float = query_rows.astype(jnp.float32)
    reach = cumulative + start_max[:, None]
    new_max = jnp.maximum(local_max, reach)
    own_scale = jnp.transpose(jnp.exp(local_max - new_max))
    past_scale = jnp.transpose(jnp.exp(reach - new_max)) * scaling
    from_memory = jnp.einsum('thk,hvk->thv', query_float, memory, precision=lax.Precision.HIGHEST)
    from_normer = jnp.einsum('thk,hk->th', query_float, normer, precision=lax.Precision.HIGHEST)
    numerator = own_scale[:, :, None] * local_num + past_scale[:, :, None] * from_memory
    denominator = own_scale * jnp.transpose(local_den) + past_scale * from_normer
    return numerator / jnp.maximum(jnp.abs(denominator), 1.0)[:, :, None]

def direction_outputs(query_rows, key_rows, value_rows, in_gate, log_forget):
    count = query_rows.shape[0] // TOK_DEV
    number_of_heads = query_rows.shape[1]
    head_width = query_rows.shape[2]

    def blocks(packed):
        return packed.reshape((count, TOK_DEV) + packed.shape[1:])

    def gate_blocks(packed):
        return jnp.moveaxis(packed.reshape(number_of_heads, count, TOK_DEV), 1, 0)

    def block_step(carried, block_inputs):
        queries, key_block, value_block, gate_block, forget_block = block_inputs
        local, summary = local_pass(queries, key_block, value_block, gate_block, forget_block)
        return (combine(carried, summary), finish(local, queries, carried))
    inputs = (blocks(query_rows), blocks(key_rows), blocks(value_rows), gate_blocks(in_gate), gate_blocks(log_forget))
    final_state, outputs = lax.scan(block_step, empty_state(number_of_heads, head_width), inputs)
    return outputs.reshape(query_rows.shape)

def group_cell(query_all, every_key_row, values_all, outgate_all, gate_pre, head_width):
    token_count = query_all.shape[0]
    queries = query_all.reshape(token_count, -1, head_width)
    key_rows = every_key_row.reshape(token_count, -1, head_width)
    value_rows = values_all.reshape(token_count, -1, head_width)
    forward_out = direction_outputs(queries, key_rows, value_rows, gate_pre[0], jax.nn.log_sigmoid(gate_pre[2]))
    backward_out = direction_outputs(queries[::-1], key_rows[::-1], value_rows[::-1], gate_pre[1][:, ::-1], jax.nn.log_sigmoid(gate_pre[3])[:, ::-1])[::-1]
    summed = forward_out + backward_out
    normed = summed * lax.rsqrt(lax.optimization_barrier(jnp.mean(summed * summed, axis=2, keepdims=True)) + EPSILON)
    return (normed.reshape(token_count, -1) * jax.nn.sigmoid(outgate_all.astype(jnp.float32))).astype(jnp.bfloat16)

def reference(residual, query_narrow, keys_narrow, values_narrow, outgate_narrow, gates_narrow, query_broad, keys_broad, values_broad, outgate_broad, gates_broad, outproj_narrow, outproj_broad, norm_gain, gate_weight, up_weight, down_weight):
    cell_narrow = group_cell(query_narrow, keys_narrow, values_narrow, outgate_narrow, gates_narrow, DH_A)
    cell_broad = group_cell(query_broad, keys_broad, values_broad, outgate_broad, gates_broad, DH_B)
    narrow_part = cell_narrow.shape[1] // N_TP
    broad_part = cell_broad.shape[1] // N_TP
    hidden_part = gate_weight.shape[1] // N_TP
    proj = jnp.zeros(residual.shape, jnp.float32)
    for member in range(N_TP):
        narrow_cols = slice(member * narrow_part, (member + 1) * narrow_part)
        broad_cols = slice(member * broad_part, (member + 1) * broad_part)
        partial_value = jnp.dot(cell_narrow[:, narrow_cols], outproj_narrow[narrow_cols], preferred_element_type=jnp.float32)
        partial_value = partial_value + jnp.dot(cell_broad[:, broad_cols], outproj_broad[broad_cols], preferred_element_type=jnp.float32)
        proj = proj + rounded(partial_value)
    stream = residual.astype(jnp.float32) + proj
    scaled = stream * lax.rsqrt(lax.optimization_barrier(jnp.mean(stream * stream, axis=1, keepdims=True)) + EPSILON)
    normed = (scaled * norm_gain.astype(jnp.float32)).astype(jnp.bfloat16)
    ffn = jnp.zeros(residual.shape, jnp.float32)
    for member in range(N_TP):
        hidden_cols = slice(member * hidden_part, (member + 1) * hidden_part)
        gate = jnp.dot(normed, gate_weight[:, hidden_cols], preferred_element_type=jnp.float32)
        upward = jnp.dot(normed, up_weight[:, hidden_cols], preferred_element_type=jnp.float32)
        hidden = (jax.nn.silu(gate) * upward).astype(jnp.bfloat16)
        partial_value = lax.dot_general(hidden, down_weight[:, hidden_cols], (((1,), (1,)), ((), ())), preferred_element_type=jnp.float32)
        ffn = ffn + rounded(partial_value)
    return (stream + 0.5 * ffn).astype(jnp.bfloat16)
```

```python
import functools

import jax
import jax.numpy as jnp
from jax import lax
from jax.experimental import pallas as pl
from jax.experimental.pallas import tpu as pltpu
from jax.sharding import PartitionSpec as P

DH_A = 128
DH_B = 256


EPSILON = 1e-06
START_MAX = -1e30
MASKED = -1e38


VMEM = pl.BlockSpec(memory_space=pltpu.VMEM)
SMEM = pl.BlockSpec(memory_space=pltpu.SMEM)
F32 = jnp.float32
BF16 = jnp.bfloat16


def call(body, outs, *args, scratch=(), flops=2**22, name=None):
    specs = [SMEM if a.dtype == jnp.int32 else VMEM for a in args]
    return pl.pallas_call(
        body,
        out_shape=outs,
        in_specs=specs,
        out_specs=jax.tree.map(lambda _: VMEM, outs),
        scratch_shapes=scratch,
        cost_estimate=pl.CostEstimate(flops=flops, transcendentals=0, bytes_accessed=2**20),
        compiler_params=pltpu.CompilerParams(vmem_limit_bytes=48 * 2**20),
        name=name,
    )(*args)


def shaped(shape, dtype):
    return jax.ShapeDtypeStruct(shape, dtype)


def nt(a, b):
    return lax.dot_general(a, b, (((1,), (1,)), ((), ())), preferred_element_type=F32)


def nn(a, b):
    return lax.dot_general(a, b, (((1,), (0,)), ((), ())), preferred_element_type=F32)


def lanes_of(x):
    return lax.broadcasted_iota(jnp.int32, x.shape, 1)


def prefix(x):
    lane, step = lanes_of(x), 1
    while step < x.shape[1]:
        x = x + jnp.where(lane >= step, pltpu.roll(x, step, 1), 0.0)
        step *= 2
    return x


def suffix(x):
    lane, step, width = lanes_of(x), 1, x.shape[1]
    while step < width:
        x = x + jnp.where(lane < width - step, pltpu.roll(x, width - step, 1), 0.0)
        step *= 2
    return x


def log_sigmoid(x):
    return jnp.minimum(x, 0.0) - jnp.log1p(jnp.exp(-jnp.abs(x)))


def gate_rows(narrow_ref, broad_ref, rows_ref):
    narrow = narrow_ref.shape[1]
    heads = narrow + broad_ref.shape[1]
    rows_ref[...] = jnp.zeros_like(rows_ref)
    for role in range(4):
        rows_ref[role, 0:narrow, :] = narrow_ref[role]
        rows_ref[role, narrow:heads, :] = broad_ref[role]
    return rows_ref[0], rows_ref[1], log_sigmoid(rows_ref[2]), log_sigmoid(rows_ref[3])


def three_parts(x):
    high = x.astype(BF16)
    rest = x - high.astype(F32)
    middle = rest.astype(BF16)
    return high, middle, (rest - middle.astype(F32)).astype(BF16)


def pack_body(kn, vn, kb, vb, gates_n, gates_b, out, rows_ref):
    length, width = kn.shape
    for at, ref in enumerate((kn, vn, kb, vb)):
        out[0:length, at * width : (at + 1) * width] = ref[...]
    in_f, in_b, lf, lb = gate_rows(gates_n, gates_b, rows_ref)
    lane = lanes_of(lf)
    run_b = prefix(lb)
    after = jnp.where(lane < length - 1, pltpu.roll(suffix(lf), length - 1, 1), 0.0)
    before = jnp.where(lane >= 1, pltpu.roll(run_b, 1, 1), 0.0)
    total_f = jnp.broadcast_to(prefix(lf)[:, length - 1 : length], lf.shape)
    total_b = jnp.broadcast_to(run_b[:, length - 1 : length], lb.shape)
    first = jnp.concatenate([after + in_f, before + in_b], axis=0)
    second = jnp.concatenate([total_f, total_b], axis=0)
    at = 0
    for a, b in zip(three_parts(first), three_parts(second)):
        out[length : length + 16, at : at + length] = a
        out[length : length + 16, at + length : at + 2 * length] = b
        at += 2 * length
    out[length : length + 16, at:] = jnp.zeros((16, 4 * width - at), BF16)


def unpack(ref, length):
    rows = ref[length : length + 16, 0 : 6 * length].astype(F32)
    part = [rows[:, k * length : (k + 1) * length] for k in range(6)]
    first = part[0] + (part[2] + part[4])
    second = part[1] + (part[3] + part[5])
    return first[0:8], first[8:16], second[0:8], second[8:16]


def head_list(width_a, width_b):
    heads = []
    for start, width, size in ((0, width_a, DH_A), (2 * width_a, width_b, DH_B)):
        out_start = 0 if start == 0 else width_a
        for k in range(width // size):
            heads.append(
                (start + k * size, start + width + k * size, out_start + k * size, size)
            )
    return heads


def flag(condition):
    return jnp.where(condition, 1.0, 0.0).astype(F32)


def state_body(near, width_a, width_b, place, *refs):
    bufs, out, extra = refs[:near], refs[near], refs[near + 1]
    length = bufs[0].shape[0] - 16
    s = place[0]
    p, first_half = s & (near - 1), s < near
    rows = []
    for ref in bufs:
        gl_f, gl_b, tot_f, tot_b = unpack(ref, length)
        rows.append((jnp.where(first_half, gl_f, gl_b), jnp.where(first_half, tot_f, tot_b)))
    reach = []
    for k in range(near):
        g = rows[k][0]
        for o in range(near):
            if o != k:
                later = jnp.where(first_half, (p ^ o) > (p ^ k), (p ^ o) < (p ^ k))
                g = g + flag(later) * rows[o][1]
        reach.append(g)
    top = reach[0]
    for g in reach[1:]:
        top = jnp.maximum(top, g)
    top = jnp.max(top, axis=1, keepdims=True)
    share = [jnp.transpose(jnp.exp(g - top)) for g in reach]
    extra[...] = jnp.zeros_like(extra)
    row_at = 0
    for h, (klane, vlane, olane, size) in enumerate(head_list(width_a, width_b)):
        memory, norm = None, None
        for k in range(near):
            keys = bufs[k][0:length, klane : klane + size].astype(F32) * share[k][:, h : h + 1]
            values = bufs[k][0:length, vlane : vlane + size]
            part = lax.dot_general(
                keys.astype(BF16), values, (((0,), (0,)), ((), ())), preferred_element_type=F32
            )
            count = jnp.sum(keys, axis=0, keepdims=True)
            memory = part if memory is None else memory + part
            norm = count if norm is None else norm + count
        group = 0 if olane < width_a else 1
        row_at = 0 if group == 0 else DH_A
        lane = olane - group * width_a
        out[row_at : row_at + size, lane : lane + size] = memory.astype(BF16)
        extra[group : group + 1, lane : lane + size] = norm
        extra[2 + h : 3 + h, :] = jnp.broadcast_to(top[h : h + 1, :], (1, extra.shape[1]))
    base = DH_A + DH_B
    for k, part in enumerate(three_parts(extra[...])):
        out[base + 16 * k : base + 16 * (k + 1), :] = part


def near_body(near, width_a, width_b, place, *refs):
    q_n, q_b, gates_n, gates_b = refs[:4]
    bufs = refs[4 : 4 + near]
    done_ref, num_ref, stat_ref, rows_ref = refs[4 + near :]
    length = q_n.shape[0]
    s = place[0]
    p, first_half = s & (near - 1), s < near
    in_f, in_b, lf, lb = gate_rows(gates_n, gates_b, rows_ref)
    cum_f, cum_b = prefix(lf), suffix(lb)
    col_f, col_b = jnp.transpose(cum_f), jnp.transpose(cum_b)
    rows = [unpack(ref, length) for ref in bufs]
    is_f, reach = [None], [None]
    for k in range(1, near):
        ahead = (p ^ k) < p
        is_f.append(flag(ahead))
        g = jnp.where(ahead, rows[k][0], rows[k][1])
        for o in range(1, near):
            if o != k:
                between_f = jnp.logical_and((p ^ o) > (p ^ k), (p ^ o) < p)
                between_b = jnp.logical_and((p ^ o) < (p ^ k), (p ^ o) > p)
                g = g + flag(jnp.logical_and(ahead, between_f)) * rows[o][2]
                g = g + flag(jnp.logical_and(jnp.logical_not(ahead), between_b)) * rows[o][3]
        reach.append(g)
    in_max = []
    for forward in (True, False):
        top = jnp.full((8, 1), START_MAX, F32)
        for k in range(1, near):
            keep = (is_f[k] > 0.5) if forward else (is_f[k] < 0.5)
            top = jnp.maximum(
                top, jnp.where(keep, jnp.max(reach[k], axis=1, keepdims=True), START_MAX)
            )
        in_max.append(top)
    share = [None] + [
        jnp.exp(reach[k] - jnp.where(is_f[k] > 0.5, in_max[0], in_max[1])) for k in range(1, near)
    ]
    edge = jnp.zeros_like(lf)
    for o in range(1, near):
        edge = edge + flag(jnp.logical_and(jnp.logical_not(first_half), (p ^ o) < p)) * rows[o][2]
        edge = edge + flag(jnp.logical_and(first_half, (p ^ o) > p)) * rows[o][3]
    to_edge = jnp.where(first_half, col_b, col_f) + jnp.transpose(edge)
    t = lax.broadcasted_iota(jnp.int32, (length, length), 0)
    u = lax.broadcasted_iota(jnp.int32, (length, length), 1)
    lane = lax.broadcasted_iota(jnp.int32, stat_ref.shape, 1)
    stat = jnp.zeros(stat_ref.shape, F32)
    for h, (klane, vlane, olane, size) in enumerate(head_list(width_a, width_b)):
        q_ref, at = (q_n, olane) if olane < width_a else (q_b, olane - width_a)
        q = q_ref[:, at : at + size]
        scaling = size ** (-0.5)
        own_v = bufs[0][0:length, vlane : vlane + size]
        own_s = nt(q, bufs[0][0:length, klane : klane + size]) * scaling
        past_num, past_den = [None, None], [None, None]
        for k in range(1, near):
            scores = nt(q, bufs[k][0:length, klane : klane + size]) * scaling
            scores = scores * share[k][h : h + 1, :]
            num = nn(scores.astype(BF16), bufs[k][0:length, vlane : vlane + size])
            den = jnp.sum(scores, axis=1, keepdims=True)
            for d, weight in enumerate((is_f[k], 1.0 - is_f[k])):
                past_num[d] = weight * num if k == 1 else past_num[d] + weight * num
                past_den[d] = weight * den if k == 1 else past_den[d] + weight * den
        found = []
        for d, (col, row, gate, keep) in enumerate(
            ((col_f, cum_f, in_f, t >= u), (col_b, cum_b, in_b, t <= u))
        ):
            c = col[:, h : h + 1]
            w = jnp.where(keep, c - row[h : h + 1, :] + gate[h : h + 1, :], MASKED)
            past = c + in_max[d][h : h + 1, :]
            top = jnp.maximum(jnp.max(w, axis=1, keepdims=True), past)
            weighted = jnp.exp(w - top) * own_s
            if near > 1:
                scale_past = jnp.exp(past - top)
                num = nn(weighted.astype(BF16), own_v) + scale_past * past_num[d]
                den = jnp.sum(weighted, axis=1, keepdims=True) + scale_past * past_den[d]
            else:
                num = nn(weighted.astype(BF16), own_v)
                den = jnp.sum(weighted, axis=1, keepdims=True)
            found.append((num, den, top))
        (num_f, den_f, top_f), (num_b, den_b, top_b) = found
        closed = jnp.where(first_half, num_f, num_b)
        closed_den = jnp.where(first_half, den_f, den_b)
        done_ref[:, olane : olane + size] = closed / jnp.maximum(jnp.abs(closed_den), 1.0)
        num_ref[:, olane : olane + size] = jnp.where(first_half, num_b, num_f)
        stat = jnp.where(lane == h, jnp.where(first_half, den_b, den_f), stat)
        stat = jnp.where(lane == 8 + h, jnp.where(first_half, top_b, top_f), stat)
        stat = jnp.where(lane == 16 + h, to_edge[:, h : h + 1], stat)
    stat_ref[...] = stat


def join_body(parts, width_a, width_b, place, *refs):
    q_n, q_b, gate_n, gate_b, done_ref, num_ref, stat_ref, far, w_n, w_b = refs[:10]
    outs, cell_ref, proj_ref = refs[10 : 10 + parts], refs[10 + parts], refs[11 + parts]
    j = place[1]
    base = DH_A + DH_B
    extra = (
        far[base : base + 16, :].astype(F32)
        + far[base + 16 : base + 32, :].astype(F32)
        + far[base + 32 : base + 48, :].astype(F32)
    )
    for h, (_, _, olane, size) in enumerate(head_list(width_a, width_b)):
        group = 0 if olane < width_a else 1
        at = olane - group * width_a
        q = (q_n, q_b)[group][:, at : at + size]
        scaling = size ** (-0.5)
        row = 0 if group == 0 else DH_A
        from_memory = nn(q, far[row : row + size, at : at + size]) * scaling
        from_norm = (
            jnp.sum(q.astype(F32) * extra[group : group + 1, at : at + size], axis=1, keepdims=True)
            * scaling
        )
        den, top = stat_ref[:, h : h + 1], stat_ref[:, 8 + h : 9 + h]
        reach = stat_ref[:, 16 + h : 17 + h] + extra[2 + h : 3 + h, 0:1]
        new_top = jnp.maximum(top, reach)
        keep, add = jnp.exp(top - new_top), jnp.exp(reach - new_top)
        num = keep * num_ref[:, olane : olane + size] + add * from_memory
        den = keep * den + add * from_norm
        y = num / jnp.maximum(jnp.abs(den), 1.0) + done_ref[:, olane : olane + size]
        y = y * lax.rsqrt(jnp.mean(y * y, axis=1, keepdims=True) + EPSILON)
        pre = (gate_n, gate_b)[group][:, at : at + size].astype(F32)
        cell_ref[:, olane : olane + size] = (y * jax.nn.sigmoid(pre)).astype(BF16)
    proj_ref[...] = (
        nn(cell_ref[:, 0:width_a], w_n[...]) + nn(cell_ref[:, width_a:], w_b[...])
    ).astype(BF16)
    count = outs[0].shape[0]
    for k, out in enumerate(outs):
        start = pl.multiple_of((j ^ k) * count, count)
        out[...] = proj_ref[pl.ds(start, count), :]


def stream_body(parts, place, residual, gain, *refs):
    pieces, stream_ref, normed_ref = refs[:parts], refs[parts], refs[parts + 1]
    count = stream_ref.shape[0]
    start = pl.multiple_of(place[1] * count, count)
    stream = residual[pl.ds(start, count), :].astype(F32)
    proj = pieces[0][...].astype(F32)
    for piece in pieces[1:]:
        proj = proj + piece[...].astype(F32)
    stream = stream + proj
    stream_ref[...] = stream
    scaled = stream * lax.rsqrt(jnp.mean(stream * stream, axis=1, keepdims=True) + EPSILON)
    normed_ref[...] = (scaled * gain[...].astype(F32)).astype(BF16)


def turn_body(parts, place, gate, up, down, *refs):
    outs, turned = refs[:parts], refs[parts]
    s = place[0]
    count = outs[0].shape[0] // 3
    for at, ref in enumerate((gate, up, down)):
        turned[at] = jnp.transpose(ref[...])
    for k, out in enumerate(outs):
        start = pl.multiple_of((s ^ k) * count, count)
        for at in range(3):
            out[at * count : (at + 1) * count, :] = turned[at, pl.ds(start, count), :]


def mixer_body(blocks, shares, place, *refs):
    xs = refs[:blocks]
    weights = refs[blocks : blocks + blocks * shares]
    outs = refs[blocks + blocks * shares : 2 * blocks + blocks * shares]
    x_ref, out_ref = refs[2 * blocks + blocks * shares :]
    s = place[0]
    rows = xs[0].shape[0]
    count, width = weights[0].shape[0] // 3, weights[0].shape[1]
    for k in range(blocks):
        x_ref[k * rows : (k + 1) * rows, :] = xs[k][...]
    hidden = []
    for g in range(shares):
        acc = None
        for k in range(blocks):
            start = pl.multiple_of((s ^ k) * width, width)
            part = nt(x_ref[:, pl.ds(start, width)], weights[g * blocks + k][0 : 2 * count, :])
            acc = part if acc is None else acc + part
        gate, up = acc[:, 0:count], acc[:, count:]
        hidden.append((gate * jax.nn.sigmoid(gate) * up).astype(BF16))
    for k in range(blocks):
        acc = None
        for g in range(shares):
            part = nn(hidden[g], weights[g * blocks + k][2 * count :, :])
            acc = part if acc is None else acc + part
        start = pl.multiple_of((s ^ k) * width, width)
        out_ref[:, pl.ds(start, width)] = acc.astype(BF16)
    for k in range(blocks):
        outs[k][...] = out_ref[k * rows : (k + 1) * rows, :]


def final_body(parts, stream, *refs):
    pieces, out = refs[:parts], refs[parts]
    ffn = pieces[0][...].astype(F32)
    for piece in pieces[1:]:
        ffn = ffn + piece[...].astype(F32)
    out[...] = (stream[...] + 0.5 * ffn).astype(BF16)


def swap(x, axis, k):
    return lax.ppermute(x, axis, [(i, i ^ k) for i in range(lax.axis_size(axis))])


def exchanged(
    residual,
    query_narrow,
    keys_narrow,
    values_narrow,
    outgate_narrow,
    gates_narrow,
    query_broad,
    keys_broad,
    values_broad,
    outgate_broad,
    gates_broad,
    outproj_narrow,
    outproj_broad,
    norm_gain,
    gate_weight,
    up_weight,
    down_weight,
):
    blocks, shares = lax.axis_size("sp"), lax.axis_size("tp")
    near = blocks // 2
    length, width_a = query_narrow.shape
    width_b = query_broad.shape[1]
    model = residual.shape[1]
    count = length // shares
    place = jnp.stack([lax.axis_index("sp"), lax.axis_index("tp")]).astype(jnp.int32)

    rows = pltpu.VMEM((4, 8, length), F32)
    packed = call(
        pack_body,
        shaped((length + 16, 2 * width_a + 2 * width_b), BF16),
        keys_narrow, values_narrow, keys_broad, values_broad, gates_narrow, gates_broad,
        scratch=[rows],
        name="pack",
    )
    bufs = [packed] + [swap(packed, "sp", k) for k in range(1, near)]

    hidden_rows = gate_weight.shape[1] // blocks
    piece = shaped((3 * hidden_rows, gate_weight.shape[0]), BF16)
    turned = call(
        functools.partial(turn_body, blocks),
        [piece] * blocks,
        place, gate_weight, up_weight, down_weight,
        scratch=[pltpu.VMEM((3, gate_weight.shape[1], gate_weight.shape[0]), BF16)],
        name="turn",
    )
    order = list(range(near, blocks)) + list(range(1, near))
    weights = [turned[0]] + [None] * (blocks - 1)
    for k in order:
        weights[k] = swap(turned[k], "sp", k)

    state = call(
        functools.partial(state_body, near, width_a, width_b),
        shaped((DH_A + DH_B + 48, width_a), BF16),
        place, *bufs,
        scratch=[pltpu.VMEM((16, width_a), F32)],
        name="state",
    )
    far = swap(state, "sp", near)
    done, num, stat = call(
        functools.partial(near_body, near, width_a, width_b),
        [
            shaped((length, width_a + width_b), F32),
            shaped((length, width_a + width_b), F32),
            shaped((length, 128), F32),
        ],
        place, query_narrow, query_broad, gates_narrow, gates_broad, *bufs,
        scratch=[rows],
        name="near",
    )
    parts = call(
        functools.partial(join_body, shares, width_a, width_b),
        [shaped((count, model), BF16)] * shares,
        place, query_narrow, query_broad, outgate_narrow, outgate_broad, done, num, stat, far,
        outproj_narrow, outproj_broad,
        scratch=[
            pltpu.VMEM((length, width_a + width_b), BF16),
            pltpu.VMEM((length, model), BF16),
        ],
        name="join",
    )
    parts = [parts[0]] + [swap(parts[k], "tp", k) for k in range(1, shares)]
    stream, normed = call(
        functools.partial(stream_body, shares),
        [shaped((count, model), F32), shaped((count, model), BF16)],
        place, residual, norm_gain.reshape(1, -1), *parts,
        name="stream",
    )
    rows_in = [normed] + [swap(normed, "sp", k) for k in range(1, blocks)]

    bit = shares // 2
    while bit:
        weights = weights + [swap(w, "tp", bit) for w in weights]
        bit //= 2
    outs = call(
        functools.partial(mixer_body, blocks, shares),
        [shaped((count, model), BF16)] * blocks,
        place, *rows_in, *weights,
        scratch=[
            pltpu.VMEM((blocks * count, model), BF16),
            pltpu.VMEM((blocks * count, model), BF16),
        ],
        name="mixer",
    )
    pieces = [outs[0]] + [swap(outs[k], "sp", k) for k in range(1, blocks)]
    return call(
        functools.partial(final_body, blocks),
        shaped((count, model), BF16),
        stream, *pieces,
        name="final",
    )


def aligned(mesh, args):
    blocks, shares = mesh.shape["sp"], mesh.shape["tp"]
    length = args[0].shape[0] // blocks
    width = args[1].shape[1] // shares
    return (
        blocks > 1
        and blocks & (blocks - 1) == 0
        and shares & (shares - 1) == 0
        and length == 128
        and length % (16 * shares) == 0
        and width == args[6].shape[1] // shares
        and width % DH_A == 0
        and width % DH_B == 0
        and width // DH_A + width // DH_B <= 8
        and 4 * width >= 6 * length
        and args[14].shape[1] % (16 * blocks * shares) == 0
        and args[14].shape[0] % (128 * blocks) == 0
    )


def carried_in(x, axis, combine, identity, reverse):
    length, place = (lax.axis_size(axis), lax.axis_index(axis))
    everything = jax.tree.map(lambda part: lax.all_gather(part, axis), x)
    start = jax.tree.map(
        lambda part, zero: jnp.broadcast_to(jnp.asarray(zero, part.dtype), part.shape), x, identity
    )

    def hop(k, before):
        at = length - 1 - k if reverse else k
        reached = at > place if reverse else at < place
        new = combine(before, jax.tree.map(lambda part: part[at], everything))
        return jax.tree.map(lambda a, b: jnp.where(reached, a, b), new, before)

    return lax.fori_loop(0, length, hop, start)


def empty_state(number_of_heads, head_width):
    return (
        jnp.zeros((number_of_heads, head_width, head_width), jnp.float32),
        jnp.zeros((number_of_heads, head_width), jnp.float32),
        jnp.full((number_of_heads,), START_MAX, jnp.float32),
        jnp.zeros((number_of_heads,), jnp.float32),
    )


def combine(earlier_state, later_state):
    memory_early, normer_early, max_early, total_early = earlier_state
    memory_late, normer_late, max_late, total_late = later_state
    new_max = jnp.maximum(max_early + total_late, max_late)
    keep_early = jnp.exp(max_early + total_late - new_max)
    keep_late = jnp.exp(max_late - new_max)
    return (
        keep_early[:, None, None] * memory_early + keep_late[:, None, None] * memory_late,
        keep_early[:, None] * normer_early + keep_late[:, None] * normer_late,
        new_max,
        total_early + total_late,
    )


def combine_groups(earlier_state, later_state):
    return combine(earlier_state[:4], later_state[:4]) + combine(earlier_state[4:], later_state[4:])


def local_pass(query_rows, key_rows, value_rows, in_gate, log_forget):
    length = query_rows.shape[0]
    scaling = query_rows.shape[2] ** (-0.5)
    cumulative = jnp.cumsum(log_forget, axis=1)
    positions = jnp.arange(length)
    lower_tri = positions[:, None] >= positions[None, :]
    log_weight = jnp.where(
        lower_tri[None],
        cumulative[:, :, None] - cumulative[:, None, :] + in_gate[:, None, :],
        -jnp.inf,
    )
    local_max = jnp.max(log_weight, axis=2)
    scores = (
        jnp.einsum("thd,shd->hts", query_rows, key_rows, preferred_element_type=jnp.float32)
        * scaling
    )
    weighted = jnp.exp(log_weight - local_max[:, :, None]) * scores
    local_den = jnp.sum(weighted, axis=2)
    local_num = jnp.einsum(
        "hts,shd->thd",
        weighted.astype(jnp.bfloat16),
        value_rows,
        preferred_element_type=jnp.float32,
    )
    decay_total = cumulative[:, -1]
    toward_end = decay_total[:, None] - cumulative + in_gate
    end_max = jnp.max(toward_end, axis=1)
    end_share = jnp.exp(toward_end - end_max[:, None])
    weighted_keys = jnp.transpose(end_share)[:, :, None] * key_rows.astype(jnp.float32)
    memory = jnp.einsum(
        "shv,shk->hvk",
        value_rows,
        weighted_keys.astype(jnp.bfloat16),
        preferred_element_type=jnp.float32,
    )
    normer = jnp.sum(weighted_keys, axis=0)
    return ((local_num, local_den, local_max, cumulative), (memory, normer, end_max, decay_total))


def finish(local, query_rows, carried):
    local_num, local_den, local_max, cumulative = local
    memory, normer, start_max, decay_total = carried
    scaling = query_rows.shape[2] ** (-0.5)
    query_float = query_rows.astype(jnp.float32)
    reach = cumulative + start_max[:, None]
    new_max = jnp.maximum(local_max, reach)
    own_scale = jnp.transpose(jnp.exp(local_max - new_max))
    past_scale = jnp.transpose(jnp.exp(reach - new_max)) * scaling
    from_memory = jnp.einsum("thk,hvk->thv", query_float, memory, precision=lax.Precision.HIGHEST)
    from_normer = jnp.einsum("thk,hk->th", query_float, normer, precision=lax.Precision.HIGHEST)
    numerator = own_scale[:, :, None] * local_num + past_scale[:, :, None] * from_memory
    denominator = own_scale * jnp.transpose(local_den) + past_scale * from_normer
    return numerator / jnp.maximum(jnp.abs(denominator), 1.0)[:, :, None]


def group_passes(query_all, every_key_row, values_all, gate_pre, head_width):
    length = query_all.shape[0]
    queries = query_all.reshape(length, -1, head_width)
    key_rows = every_key_row.reshape(length, -1, head_width)
    value_rows = values_all.reshape(length, -1, head_width)
    forward = local_pass(
        queries, key_rows, value_rows, gate_pre[0], jax.nn.log_sigmoid(gate_pre[2])
    )
    backward = local_pass(
        queries[::-1],
        key_rows[::-1],
        value_rows[::-1],
        gate_pre[1][:, ::-1],
        jax.nn.log_sigmoid(gate_pre[3])[:, ::-1],
    )
    return (queries, forward, backward)


def cell_output(queries, forward, backward, state_forward, state_backward, outgate_all):
    forward_out = finish(forward[0], queries, state_forward)
    backward_out = finish(backward[0], queries[::-1], state_backward)[::-1]
    summed = forward_out + backward_out
    normed = summed * lax.rsqrt(jnp.mean(summed * summed, axis=2, keepdims=True) + EPSILON)
    length = summed.shape[0]
    return (normed.reshape(length, -1) * jax.nn.sigmoid(outgate_all.astype(jnp.float32))).astype(
        jnp.bfloat16
    )


def rms_norm(stream, norm_gain):
    scaled = stream * lax.rsqrt(jnp.mean(stream * stream, axis=1, keepdims=True) + EPSILON)
    return (scaled * norm_gain.astype(jnp.float32)).astype(jnp.bfloat16)


def shards(
    residual,
    query_narrow,
    keys_narrow,
    values_narrow,
    outgate_narrow,
    gates_narrow,
    query_broad,
    keys_broad,
    values_broad,
    outgate_broad,
    gates_broad,
    outproj_narrow,
    outproj_broad,
    norm_gain,
    gate_weight,
    up_weight,
    down_weight,
):
    narrow_rows, narrow_fwd, narrow_bwd = group_passes(
        query_narrow, keys_narrow, values_narrow, gates_narrow, DH_A
    )
    broad_rows, broad_fwd, broad_bwd = group_passes(
        query_broad, keys_broad, values_broad, gates_broad, DH_B
    )
    starting = empty_state(narrow_rows.shape[1], DH_A) + empty_state(broad_rows.shape[1], DH_B)
    into_forward = carried_in(narrow_fwd[1] + broad_fwd[1], "sp", combine_groups, starting, False)
    into_backward = carried_in(narrow_bwd[1] + broad_bwd[1], "sp", combine_groups, starting, True)
    cell_narrow = cell_output(
        narrow_rows,
        narrow_fwd,
        narrow_bwd,
        tuple(into_forward[:4]),
        tuple(into_backward[:4]),
        outgate_narrow,
    )
    cell_broad = cell_output(
        broad_rows,
        broad_fwd,
        broad_bwd,
        tuple(into_forward[4:]),
        tuple(into_backward[4:]),
        outgate_broad,
    )
    tok_rows = residual.shape[0]
    own_count = tok_rows // lax.axis_size("tp")
    offset = lax.axis_index("tp") * own_count
    proj = lax.psum(
        (
            jnp.dot(cell_narrow, outproj_narrow, preferred_element_type=jnp.float32)
            + jnp.dot(cell_broad, outproj_broad, preferred_element_type=jnp.float32)
        ).astype(jnp.bfloat16),
        "tp",
    ).astype(jnp.float32)
    stream = residual.astype(jnp.float32) + proj
    normed = rms_norm(stream, norm_gain)
    own_stream = lax.dynamic_slice_in_dim(stream, offset, own_count, 0)
    gate = jnp.dot(
        normed,
        lax.all_gather(gate_weight, "sp", axis=0, tiled=True),
        preferred_element_type=jnp.float32,
    )
    upward = jnp.dot(
        normed,
        lax.all_gather(up_weight, "sp", axis=0, tiled=True),
        preferred_element_type=jnp.float32,
    )
    hidden = (jax.nn.silu(gate) * upward).astype(jnp.bfloat16)
    partial_value = lax.dot_general(
        hidden,
        lax.all_gather(down_weight, "sp", axis=0, tiled=True),
        (((1,), (1,)), ((), ())),
        preferred_element_type=jnp.float32,
    )
    ffn = lax.psum_scatter(
        partial_value.astype(jnp.bfloat16), "tp", scatter_dimension=0, tiled=True
    ).astype(jnp.float32)
    return (own_stream + 0.5 * ffn).astype(jnp.bfloat16)


def solution(mesh):
    in_specs = (
        P("sp", None),
        P("sp", "tp"),
        P("sp", "tp"),
        P("sp", "tp"),
        P("sp", "tp"),
        P(None, "tp", "sp"),
        P("sp", "tp"),
        P("sp", "tp"),
        P("sp", "tp"),
        P("sp", "tp"),
        P(None, "tp", "sp"),
        P("tp", None),
        P("tp", None),
        P(),
        P("sp", "tp"),
        P("sp", "tp"),
        P("sp", "tp"),
    )
    out_specs = P(("sp", "tp"), None)

    def whole(*args):
        body = exchanged if aligned(mesh, args) else shards
        return jax.shard_map(
            body, mesh=mesh, in_specs=in_specs, out_specs=out_specs, check_vma=False
        )(*args)

    return whole
```
